32 devices in a mesh: ep: 8 (over z, x), tp: 4 (over y, core).
Axes of the slice: x: 2, y: 2, z: 4, core: 2. Of those that a mesh axis runs over, the one named last changes fastest.
Arguments:
- hidden_in: bfloat16 [128, 2048], P(None, 'ep'), may hold values from -24 to 24
- attn_gain: float32 [2048], replicated, may hold values from 0.1 to 1.9
- forget_weight: bfloat16 [2048, 16], replicated, may hold values from -0.125 to 0.125
- forget_bias: float32 [16], replicated, may hold values from -1 to 2
- query_weight: bfloat16 [2048, 2048], P('ep', 'tp'), may hold values from -0.125 to 0.125
- key_weight: bfloat16 [2048, 1024], P('ep', 'tp'), may hold values from -0.125 to 0.125
- value_weight: bfloat16 [2048, 1024], P('ep', 'tp'), may hold values from -0.125 to 0.125
- query_gain: float32 [128], replicated, may hold values from 0.1 to 1.9
- key_gain: float32 [128], replicated, may hold values from 0.1 to 1.9
- cache_keys: bfloat16 [128, 8, 1024, 128], P('ep', 'tp'), may hold values from -160 to 160
- cache_values: bfloat16 [128, 8, 1024, 128], P('ep', 'tp'), may hold values from -6 to 6
- cache_gates: float32 [128, 16, 1024], P('ep', 'tp'), may hold values from -256 to 0, as said below
- lengths: int32 [128], P('ep'), may hold values from 128 to 1024, as said below
- output_weight: bfloat16 [2048, 2048], P('tp', 'ep'), may hold values from -0.125 to 0.125
- ffn_gain: float32 [2048], replicated, may hold values from 0.1 to 1.9
- route_group: int32 [128], replicated, may hold values from 0 to 3, as said below
- route_expert: int32 [128, 2], replicated, may hold values from 0 to 3, as said below
- route_weight: float32 [128, 2], replicated, may hold values from 0.1 to 0.6
- expert_gate: bfloat16 [16, 2048, 1024], P('ep', None, 'tp'), may hold values from -0.125 to 0.125
- expert_up: bfloat16 [16, 2048, 1024], P('ep', None, 'tp'), may hold values from -0.125 to 0.125
- expert_down: bfloat16 [16, 1024, 2048], P('ep', 'tp'), may hold values from -0.1875 to 0.1875
- mix_vector: bfloat16 [2048], replicated, may hold values from -0.125 to 0.125
- dense_gate: bfloat16 [2048, 4096], P('ep', 'tp'), may hold values from -0.125 to 0.125
- dense_up: bfloat16 [2048, 4096], P('ep', 'tp'), may hold values from -0.125 to 0.125
- dense_down: bfloat16 [4096, 2048], P('tp', 'ep'), may hold values from -0.09375 to 0.09375
Outputs:
- mixed: bfloat16 [128, 2048], P(None, 'ep')
- fresh_keys: bfloat16 [128, 1024], P('ep', 'tp')
- fresh_values: bfloat16 [128, 1024], P('ep', 'tp')
The draws below stay inside these ranges and needn't reach their ends.
Inputs may be any that keep to these rules, and one draw needn't show every extreme that they name: `cache_gates`: never rising along positions. `lengths`: some device holds a sequence of length 1024 in every draw. `route_group`: no expert is chosen by more than 24 tokens of the batch, and some expert by exactly 24. `route_expert`: a token's 2 experts differ; the loads of the experts of one group differ by at most two.
All inputs are finite; a program needn't handle non-finite values.
Results may differ from the reference program's by a relative error of at most 0.008.
Values may be sent and summed in bfloat16 or wider, within the bound.
A program may use at most 64 MiB of HBM per device.

```python
import jax
import jax.numpy as jnp
from jax import lax

D = 2048
QUERY_HEADS = 16
KV_HEADS = 8
HEAD_DIM = 128
EXPERT_WIDTH = 1024
DENSE_WIDTH = 4096
GROUP_EXPERTS = 4
TOPK = 2
SEQ_DEV = 16
CACHE_POSITIONS = 1024
SEQUENCE_COUNT = 128
EXPERTS = 16
GROUPS = 4
CAPACITY = 24


def draw_hidden_in(key, part):
    key_col, key_val = jax.random.split(key, 2)
    position = jnp.arange(D, dtype=jnp.float32) / D
    noise_level = jax.random.uniform(key_col, (D,), jnp.float32, 0.6, 1.4)
    column_scale = 3.0 ** position * noise_level * 0.6
    values = jax.random.normal(key_val, (SEQUENCE_COUNT, D), jnp.float32) * column_scale
    return jnp.clip(values, -24.0, 24.0).astype(jnp.bfloat16)


def draw_cache_keys(key, part):
    key_val = jax.random.fold_in(key, 0)
    values = jax.random.normal(key_val, (SEQUENCE_COUNT, KV_HEADS, CACHE_POSITIONS, HEAD_DIM), jnp.float32)
    return jnp.clip(values, -160.0, 160.0).astype(jnp.bfloat16)


def draw_cache_gates(key, part):
    kind_random_key, fast_random_key, slow_random_key, rough_random_key, spike_random_key, depth_random_key = jax.random.split(key, 6)
    chooser = jax.random.uniform(kind_random_key, (SEQUENCE_COUNT, QUERY_HEADS, 1), jnp.float32)
    fast_flag = chooser < 0.5
    fast_rate = 1.0 / jax.random.uniform(fast_random_key, (SEQUENCE_COUNT, QUERY_HEADS, 1), jnp.float32, 10.0, 40.0)
    slow_rate = jax.random.uniform(slow_random_key, (SEQUENCE_COUNT, QUERY_HEADS, 1), jnp.float32, 0.3, 1.5) / CACHE_POSITIONS
    drift_rate = jnp.where(fast_flag, fast_rate, slow_rate)
    noise_level = jax.random.uniform(rough_random_key, (SEQUENCE_COUNT, QUERY_HEADS, CACHE_POSITIONS), jnp.float32, 0.3, 1.7)
    spike_position = jax.random.uniform(spike_random_key, (SEQUENCE_COUNT, QUERY_HEADS, CACHE_POSITIONS), jnp.float32) < 3.0 / CACHE_POSITIONS
    spike_depth = jnp.log(jax.random.uniform(depth_random_key, (SEQUENCE_COUNT, QUERY_HEADS, CACHE_POSITIONS), jnp.float32, 0.5, 0.8))
    step_increments = -drift_rate * noise_level + jnp.where(spike_position & jnp.logical_not(fast_flag), spike_depth, 0.0)
    return jnp.cumsum(step_increments, axis=2).astype(jnp.float32)


def draw_lengths(key, part):
    key_len, key_pick = jax.random.split(key)
    drawn = jax.random.randint(key_len, (SEQUENCE_COUNT,), CACHE_POSITIONS // 8, CACHE_POSITIONS + 1)
    block_count = SEQUENCE_COUNT // SEQ_DEV
    picked = jax.random.randint(key_pick, (block_count, 1), 0, SEQ_DEV)
    full_length = jnp.arange(SEQ_DEV, dtype=jnp.int32)[None, :] == picked
    return jnp.where(full_length.reshape(SEQUENCE_COUNT), CACHE_POSITIONS, drawn).astype(jnp.int32)


def route_tables(key):
    folded = jax.random.fold_in(key, 11)
    key_size, key_label, key_token, key_expert = jax.random.split(folded, 4)
    mean_size = SEQUENCE_COUNT // GROUPS
    half_size = mean_size // 2
    swings = jax.random.randint(key_size, ((GROUPS - 2) // 2,), 0, half_size + 1)
    group_sizes = jnp.concatenate([jnp.array([mean_size + half_size, mean_size - half_size], jnp.int32), mean_size + swings, mean_size - swings]).astype(jnp.int32)
    group_sizes = group_sizes[jax.random.permutation(key_label, GROUPS)]
    group_ends = jnp.cumsum(group_sizes)
    starts = group_ends - group_sizes
    token_rank = jax.random.permutation(key_token, SEQUENCE_COUNT).astype(jnp.int32)
    group_of = jnp.sum((token_rank[:, None] >= group_ends[None, :]).astype(jnp.int32), axis=1)
    position = token_rank - starts[group_of]
    first_pick = position % GROUP_EXPERTS
    second = (first_pick + 1 + position // GROUP_EXPERTS % (GROUP_EXPERTS - 1)) % GROUP_EXPERTS
    labels = jax.vmap(lambda subkey: jax.random.permutation(subkey, GROUP_EXPERTS))(jax.random.split(key_expert, GROUPS)).astype(jnp.int32)
    both_picks = jnp.stack([first_pick, second], axis=1)
    experts = jnp.take_along_axis(labels[group_of], both_picks, axis=1)
    return (group_of.astype(jnp.int32), experts.astype(jnp.int32))


def draw_route_group(key, part):
    return route_tables(key)[0]


def draw_route_expert(key, part):
    return route_tables(key)[1]


def levels(key, shape, cuts, low, high):
    factor_of = 1.0
    for dim, shards_of in cuts:
        steps = jax.random.uniform(jax.random.fold_in(jax.random.fold_in(key, 6), dim), (shards_of,), jnp.float32, low / len(cuts), high / len(cuts))
        factor_of = factor_of * jnp.repeat(jnp.exp(steps), shape[dim] // shards_of).reshape((-1,) + (1,) * (len(shape) - 1 - dim))
    return factor_of


def gaussian(stream_key, extent, scale, most, cuts=(), kind=jnp.bfloat16):
    values = jax.random.normal(stream_key, extent, jnp.float32) * scale
    if len(cuts) > 0:
        values = levels(stream_key, extent, cuts, -0.22, 0.18) * values
    return jnp.clip(values, min=-most, max=most).astype(kind)


def setup_inputs(seed: int = 0) -> dict:
    seeds = jax.random.split(jax.random.key(seed), 26)
    hidden_in = draw_hidden_in(jax.random.fold_in(seeds[25], 71), 0)
    attn_gain = jnp.clip(1.0 + 0.18 * jax.random.normal(seeds[1], (D,), jnp.float32), 0.1, 1.9)
    forget_weight = gaussian(seeds[2], (D, QUERY_HEADS), D ** -0.5, 0.125)
    forget_bias = jnp.clip(jax.random.uniform(seeds[3], (QUERY_HEADS,), jnp.float32, -1.0, 2.0), -1.0, 2.0)
    query_weight = gaussian(seeds[4], (D, QUERY_HEADS * HEAD_DIM), D ** -0.5, 0.125, ((0, 8), (1, 4)))
    key_weight = gaussian(seeds[5], (D, KV_HEADS * HEAD_DIM), D ** -0.5, 0.125, ((0, 8), (1, 4)))
    value_weight = gaussian(seeds[6], (D, KV_HEADS * HEAD_DIM), D ** -0.5, 0.125, ((0, 8), (1, 4)))
    query_gain = jnp.clip(1.0 + 0.18 * jax.random.normal(seeds[7], (HEAD_DIM,), jnp.float32), 0.1, 1.9)
    key_gain = jnp.clip(1.0 + 0.18 * jax.random.normal(seeds[8], (HEAD_DIM,), jnp.float32), 0.1, 1.9)
    cache_keys = draw_cache_keys(jax.random.fold_in(seeds[25], 71), 0)
    cache_values = gaussian(seeds[10], (SEQUENCE_COUNT, KV_HEADS, CACHE_POSITIONS, HEAD_DIM), 1.0, 6.0, ((0, 8), (1, 4)))
    cache_gates = draw_cache_gates(jax.random.fold_in(seeds[25], 71), 0)
    lengths = draw_lengths(jax.random.fold_in(seeds[25], 71), 0)
    output_weight = gaussian(seeds[13], (QUERY_HEADS * HEAD_DIM, D), (QUERY_HEADS * HEAD_DIM) ** -0.5, 0.125, ((0, 4), (1, 8)))
    ffn_gain = jnp.clip(1.0 + 0.18 * jax.random.normal(seeds[14], (D,), jnp.float32), 0.1, 1.9)
    route_group = draw_route_group(jax.random.fold_in(seeds[25], 71), 0)
    route_expert = draw_route_expert(jax.random.fold_in(seeds[25], 71), 0)
    route_weight = jnp.clip(jax.random.uniform(seeds[17], (SEQUENCE_COUNT, TOPK), jnp.float32, 0.1, 0.6), 0.1, 0.6)
    expert_gate = gaussian(seeds[18], (EXPERTS, D, EXPERT_WIDTH), D ** -0.5, 0.125, ((0, 8), (2, 4)))
    expert_up = gaussian(seeds[19], (EXPERTS, D, EXPERT_WIDTH), D ** -0.5, 0.125, ((0, 8), (2, 4)))
    expert_down = gaussian(seeds[20], (EXPERTS, EXPERT_WIDTH, D), EXPERT_WIDTH ** -0.5, 0.1875, ((0, 8), (1, 4)))
    mix_vector = gaussian(seeds[21], (D,), D ** -0.5, 0.125)
    dense_gate = gaussian(seeds[22], (D, DENSE_WIDTH), D ** -0.5, 0.125, ((0, 8), (1, 4)))
    dense_up = gaussian(seeds[23], (D, DENSE_WIDTH), D ** -0.5, 0.125, ((0, 8), (1, 4)))
    dense_down = gaussian(seeds[24], (DENSE_WIDTH, D), DENSE_WIDTH ** -0.5, 0.09375, ((0, 4), (1, 8)))
    return dict(hidden_in=hidden_in, attn_gain=attn_gain, forget_weight=forget_weight, forget_bias=forget_bias, query_weight=query_weight, key_weight=key_weight, value_weight=value_weight, query_gain=query_gain, key_gain=key_gain, cache_keys=cache_keys, cache_values=cache_values, cache_gates=cache_gates, lengths=lengths, output_weight=output_weight, ffn_gain=ffn_gain, route_group=route_group, route_expert=route_expert, route_weight=route_weight, expert_gate=expert_gate, expert_up=expert_up, expert_down=expert_down, mix_vector=mix_vector, dense_gate=dense_gate, dense_up=dense_up, dense_down=dense_down)


EPS = 1e-06

def head_norm(projected, gain_vec):
    return projected * lax.rsqrt(lax.optimization_barrier(jnp.mean(projected * projected, axis=-1, keepdims=True)) + EPS) * gain_vec

def slot_targets(route_group, route_expert):
    chosen = (route_group[:, None] * GROUP_EXPERTS + route_expert).reshape(-1).astype(jnp.int32)
    onehot = (chosen[:, None] == jnp.arange(EXPERTS, dtype=jnp.int32)[None, :]).astype(jnp.int32)
    before = jnp.cumsum(onehot, axis=0) - onehot
    return (chosen * CAPACITY + lax.optimization_barrier(jnp.sum(before * onehot, axis=1))).astype(jnp.int32)

def reference(hidden_in, attn_gain, forget_weight, forget_bias, query_weight, key_weight, value_weight, query_gain, key_gain, cache_keys, cache_values, cache_gates, lengths, output_weight, ffn_gain, route_group, route_expert, route_weight, expert_gate, expert_up, expert_down, mix_vector, dense_gate, dense_up, dense_down):
    stream = hidden_in.astype(jnp.float32)
    normed_in = (stream * attn_gain).astype(jnp.bfloat16)
    inv_rms = lax.rsqrt(lax.optimization_barrier(jnp.mean(stream * stream, axis=1)) + EPS)
    query_rows = head_norm(jnp.dot(normed_in, query_weight, preferred_element_type=jnp.float32).reshape(SEQUENCE_COUNT, QUERY_HEADS, HEAD_DIM), query_gain).astype(jnp.bfloat16)
    fresh_keys = head_norm(jnp.dot(normed_in, key_weight, preferred_element_type=jnp.float32).reshape(SEQUENCE_COUNT, KV_HEADS, HEAD_DIM), key_gain).astype(jnp.bfloat16)
    fresh_values = (jnp.dot(normed_in, value_weight, preferred_element_type=jnp.float32) * inv_rms[:, None]).astype(jnp.bfloat16)
    log_forget = jax.nn.log_sigmoid(jnp.dot(normed_in, forget_weight, preferred_element_type=jnp.float32) * inv_rms[:, None] + forget_bias)
    latest = jnp.take_along_axis(cache_gates, (lengths - 1).astype(jnp.int32)[:, None, None], axis=2)[:, :, 0]
    now_gate = latest + log_forget
    group_size = QUERY_HEADS // KV_HEADS
    factor = HEAD_DIM ** (-0.5)
    positions = jnp.arange(CACHE_POSITIONS, dtype=jnp.int32)

    def one_sequence(items):
        query_one, keys_one, values_one, gates_one, now_one, length_one, key_new, value_new = items
        grouped = query_one.astype(jnp.float32).reshape(KV_HEADS, group_size, HEAD_DIM)
        scores = jnp.einsum('kgd,kcd->kgc', grouped, keys_one.astype(jnp.float32)) * factor
        scores = scores + now_one.reshape(KV_HEADS, group_size, 1) - gates_one.reshape(KV_HEADS, group_size, CACHE_POSITIONS)
        scores = jnp.where(positions < length_one, scores, -jnp.inf)
        new_key = key_new.astype(jnp.float32).reshape(KV_HEADS, 1, HEAD_DIM)
        self_score = lax.optimization_barrier(jnp.sum(grouped * new_key, axis=-1)) * factor
        ceiling = jnp.maximum(lax.optimization_barrier(jnp.max(scores, axis=-1)), self_score)
        weights = jnp.exp(scores - ceiling[:, :, None])
        self_weight = jnp.exp(self_score - ceiling)
        denominator = lax.optimization_barrier(jnp.sum(weights, axis=-1)) + self_weight
        rounded = lax.optimization_barrier(weights.astype(jnp.bfloat16)).astype(jnp.float32)
        summed = jnp.einsum('kgc,kcd->kgd', rounded, values_one.astype(jnp.float32))
        summed = summed + self_weight[:, :, None] * value_new.astype(jnp.float32).reshape(KV_HEADS, 1, HEAD_DIM)
        return (summed / denominator[:, :, None]).reshape(QUERY_HEADS * HEAD_DIM).astype(jnp.bfloat16)
    heads_out = lax.map(one_sequence, (query_rows, cache_keys, cache_values, cache_gates, now_gate, lengths, fresh_keys, fresh_values.reshape(SEQUENCE_COUNT, KV_HEADS, HEAD_DIM)))
    middle = (stream + jnp.dot(heads_out, output_weight, preferred_element_type=jnp.float32)).astype(jnp.bfloat16)
    middle_f = middle.astype(jnp.float32)
    normed_mid = (middle_f * ffn_gain).astype(jnp.bfloat16)
    mid_scale = lax.rsqrt(lax.optimization_barrier(jnp.mean(middle_f * middle_f, axis=1)) + EPS)
    mix_share = jax.nn.sigmoid(mid_scale * jnp.dot(normed_mid, mix_vector, preferred_element_type=jnp.float32))
    targets = slot_targets(route_group, route_expert)
    token_ids = jnp.arange(SEQUENCE_COUNT * TOPK, dtype=jnp.int32) // TOPK
    slot_rows = jnp.zeros((EXPERTS * CAPACITY, D), jnp.bfloat16).at[targets].set(normed_mid[token_ids])
    slot_scale = jnp.zeros((EXPERTS * CAPACITY,), jnp.float32).at[targets].set(mid_scale[token_ids])

    def one_expert(items):
        block_rows, block_scale, gate_matrix, up_matrix, down_matrix = items
        gate_pre = jnp.dot(block_rows, gate_matrix, preferred_element_type=jnp.float32) * block_scale[:, None]
        up_pre = jnp.dot(block_rows, up_matrix, preferred_element_type=jnp.float32) * block_scale[:, None]
        hidden_units = (jax.nn.silu(gate_pre) * up_pre).astype(jnp.bfloat16)
        return jnp.dot(hidden_units, down_matrix, preferred_element_type=jnp.float32)
    expert_out = lax.map(one_expert, (slot_rows.reshape(EXPERTS, CAPACITY, D), slot_scale.reshape(EXPERTS, CAPACITY), expert_gate, expert_up, expert_down)).reshape(EXPERTS * CAPACITY, D)
    picked = expert_out[targets].reshape(SEQUENCE_COUNT, TOPK, D)
    routed = lax.optimization_barrier(jnp.sum(picked * route_weight[:, :, None], axis=1))
    dense_gate_pre = jnp.dot(normed_mid, dense_gate, preferred_element_type=jnp.float32) * mid_scale[:, None]
    dense_up_pre = jnp.dot(normed_mid, dense_up, preferred_element_type=jnp.float32) * mid_scale[:, None]
    dense_hidden = (jax.nn.silu(dense_gate_pre) * dense_up_pre).astype(jnp.bfloat16)
    dense_result = jnp.dot(dense_hidden, dense_down, preferred_element_type=jnp.float32)
    mixed = (middle_f + routed + mix_share[:, None] * dense_result).astype(jnp.bfloat16)
    return (mixed, fresh_keys.reshape(SEQUENCE_COUNT, KV_HEADS * HEAD_DIM), fresh_values)
```

```python
import functools

import jax
import jax.numpy as jnp
from jax import lax
from jax.experimental import pallas as pl
from jax.experimental.pallas import tpu as pltpu
from jax.sharding import PartitionSpec as P

GROUP_EXPERTS = 4
TOPK = 2
CAPACITY = 24
EPS = 1e-06
MESH = pl.DeviceIdType.MESH
F32 = jnp.float32
BF16 = jnp.bfloat16


def mm(a, b):
    return jnp.dot(a, b, preferred_element_type=F32)


def mm_nt(a, b):
    return lax.dot_general(a, b, (((1,), (1,)), ((), ())), preferred_element_type=F32)


def layer_kernel(
    n,
    t,
    hidden,
    attn_gain,
    forget_bias,
    query_gain,
    key_gain,
    ffn_gain,
    mix_vector,
    route_group,
    route_expert,
    route_weight,
    lengths,
    fw_hbm,
    wq_hbm,
    wk_hbm,
    wv_hbm,
    ck_hbm,
    cv_hbm,
    gates_hbm,
    wo_hbm,
    eg_hbm,
    eu_hbm,
    ed_hbm,
    dg_hbm,
    du_hbm,
    dd_hbm,
    mixed_out,
    fk_out,
    fv_out,
    fw,
    wq,
    wk,
    wv,
    ck,
    cv,
    gates,
    wo,
    eg,
    eu,
    ed,
    dg,
    du,
    dd,
    q_rows,
    fk_rows,
    fv_rows,
    lf_rows,
    o_rows,
    mix_rows,
    placed_scr,
    placed_t,
    slot_rows,
    qkv_send,
    qkv_recv,
    st_send,
    st_recv,
    ag_buf,
    ar_buf,
    ms_buf,
    col_stats,
    dsp_send,
    dsp_recv,
    dn_send,
    dn_recv,
    ret_send,
    ret_recv,
    dh_buf,
    ar2_buf,
    w_sem,
    k_sem,
    v_sem,
    ep_send,
    ep_recv,
    tp_send,
    tp_recv,
):
    ep = lax.axis_index("ep")
    tp = lax.axis_index("tp")
    tokens, width = hidden.shape
    own = ck.shape[0]
    kv_here = ck.shape[1]
    positions = ck.shape[2]
    head_dim = ck.shape[3]
    q_cols = wq.shape[1]
    k_cols = wk.shape[1]
    heads = q_cols // head_dim
    group = heads // kv_here
    seqs = 8 // heads
    blocks = own // seqs
    model = n * width
    hidden_units = dg.shape[1]
    local_experts = eg.shape[0]
    slots_here = local_experts * CAPACITY
    slots = n * slots_here
    factor = head_dim ** (-0.5)

    plain = [
        (fw_hbm.at[:, pl.ds(pl.multiple_of(ep * width, width), width)], fw),
        (wq_hbm, wq),
        (wk_hbm, wk),
        (wv_hbm, wv),
        (gates_hbm, gates),
        (wo_hbm, wo),
        (dg_hbm, dg),
        (du_hbm, du),
        (eg_hbm, eg),
        (eu_hbm, eu),
        (ed_hbm, ed),
        (dd_hbm, dd),
    ]
    copies = [pltpu.make_async_copy(s, d, w_sem.at[i]) for i, (s, d) in enumerate(plain)]
    (c_fw, c_wq, c_wk, c_wv, c_gates, c_wo, c_dg, c_du, c_eg, c_eu, c_ed, c_dd) = copies

    def cache_copy(i, src, dst, sem):
        part = pl.ds(i * seqs, seqs)
        return pltpu.make_async_copy(src.at[part], dst.at[part], sem.at[i])

    for c in (c_fw, c_wq, c_wk, c_wv, c_gates):
        c.start()
    for i in range(blocks):
        cache_copy(i, ck_hbm, ck, k_sem).start()
        cache_copy(i, cv_hbm, cv, v_sem).start()
    for c in (c_wo, c_dg, c_du, c_eg, c_eu, c_ed, c_dd):
        c.start()

    barrier = pltpu.get_barrier_semaphore()
    for k in range(1, n):
        pl.semaphore_signal(
            barrier, inc=1, device_id={"ep": lax.rem(ep + k, n)}, device_id_type=MESH
        )
    for k in range(1, t):
        pl.semaphore_signal(
            barrier, inc=1, device_id={"tp": lax.rem(tp + k, t)}, device_id_type=MESH
        )

    def ep_copy(phase, peer, slot, src, dst):
        return pltpu.make_async_remote_copy(
            src_ref=src,
            dst_ref=dst,
            send_sem=ep_send.at[phase, peer],
            recv_sem=ep_recv.at[phase, slot],
            device_id={"ep": peer},
            device_id_type=MESH,
        )

    def tp_copy(phase, peer, slot, src, dst):
        return pltpu.make_async_remote_copy(
            src_ref=src,
            dst_ref=dst,
            send_sem=tp_send.at[phase, peer],
            recv_sem=tp_recv.at[phase, slot],
            device_id={"tp": peer},
            device_id_type=MESH,
        )

    ep_peers = [lax.rem(ep + k, n) for k in range(1, n)]
    tp_peers = [lax.rem(tp + k, t) for k in range(1, t)]

    def ep_start(phase, src_of, dst):
        for p in ep_peers:
            ep_copy(phase, p, ep, src_of(p), dst.at[ep]).start()

    def ep_wait(phase, src_of, dst):
        for p in ep_peers:
            ep_copy(phase, p, p, src_of(p), dst.at[p]).wait()

    def tp_start(phase, buf):
        for p in tp_peers:
            tp_copy(phase, p, tp, buf.at[tp], buf.at[tp]).start()

    def tp_wait(phase, buf):
        for p in tp_peers:
            tp_copy(phase, p, p, buf.at[tp], buf.at[p]).wait()

    def own_rows(ref):
        return lambda p: ref.at[pl.ds(pl.multiple_of(p * own, own), own), :]

    my_cols = pl.ds(pl.multiple_of(ep * width, width), width)

    stream = hidden[...].astype(F32)
    normed_in = (stream * attn_gain[:, my_cols]).astype(BF16)
    c_fw.wait()
    st_send[...] = jnp.broadcast_to(
        jnp.sum(stream * stream, axis=1, keepdims=True), st_send.shape
    )
    st_send[:, 0 : fw.shape[0]] = mm_nt(normed_in, fw[...])
    pl.semaphore_wait(barrier, n - 1 + t - 1)
    ep_start(0, own_rows(st_send), st_recv)
    c_wq.wait()
    qkv_send[:, 0:q_cols] = mm(normed_in, wq[...]).astype(BF16)
    c_wk.wait()
    qkv_send[:, q_cols : q_cols + k_cols] = mm(normed_in, wk[...]).astype(BF16)
    c_wv.wait()
    qkv_send[:, q_cols + k_cols :] = mm(normed_in, wv[...]).astype(BF16)
    ep_start(1, own_rows(qkv_send), qkv_recv)

    lane = lax.broadcasted_iota(jnp.int32, (tokens, 128), 1).astype(F32)
    sub_t = lax.broadcasted_iota(jnp.int32, (128, tokens), 0)
    chosen_rows = route_group[...].astype(F32) * GROUP_EXPERTS + route_expert[...].astype(F32)
    by_token = jnp.zeros((128, tokens), F32)
    for k in range(TOPK):
        by_token = jnp.where(sub_t == k, chosen_rows[k : k + 1, :], by_token)
    by_token = jnp.transpose(by_token, (1, 0))
    chosen = [by_token[:, k : k + 1] for k in range(TOPK)]
    onehot = [(lane == c).astype(F32) for c in chosen]
    earlier = (
        lax.broadcasted_iota(jnp.int32, (tokens, tokens), 1)
        < lax.broadcasted_iota(jnp.int32, (tokens, tokens), 0)
    ).astype(F32)
    before = mm(earlier.astype(BF16), sum(onehot).astype(BF16))
    target = [
        c * CAPACITY + jnp.sum(o * before, axis=1, keepdims=True) for c, o in zip(chosen, onehot)
    ]
    slot_lane = lax.broadcasted_iota(jnp.int32, (tokens, slots), 1).astype(F32)
    placed_t[...] = sum((slot_lane == g).astype(F32) for g in target).astype(BF16)
    packed = jnp.zeros((tokens, 128), F32)
    for k in range(TOPK):
        packed = jnp.where(lane == k, target[k], packed)
    rows = jnp.transpose(packed, (1, 0))[0:8, :]
    slot_rows[...] = rows
    slot_sub = lax.broadcasted_iota(jnp.int32, (slots, tokens), 0).astype(F32)
    placed_scr[...] = sum(
        (slot_sub == rows[k : k + 1, :]).astype(F32) for k in range(TOPK)
    ).astype(BF16)

    ep_wait(0, own_rows(st_send), st_recv)
    stats = st_send[pl.ds(pl.multiple_of(ep * own, own), own), :]
    for p in ep_peers:
        stats = stats + st_recv[p]
    own_scale = lax.rsqrt(stats[:, 127:128] / model + EPS)
    stat_lane = lax.broadcasted_iota(jnp.int32, stats.shape, 1)
    bias_lane = lax.broadcasted_iota(jnp.int32, forget_bias.shape, 1)
    ep_wait(1, own_rows(qkv_send), qkv_recv)
    sums = qkv_send[pl.ds(pl.multiple_of(ep * own, own), own), :].astype(F32)
    for p in ep_peers:
        sums = sums + qkv_recv[p].astype(F32)
    fresh_keys = []
    fresh_values = []
    for j in range(kv_here):
        at = q_cols + j * head_dim
        x = sums[:, at : at + head_dim]
        x = x * lax.rsqrt(jnp.mean(x * x, axis=1, keepdims=True) + EPS) * key_gain[...]
        x = x.astype(BF16)
        fk_out[:, j * head_dim : (j + 1) * head_dim] = x
        fresh_keys.append(x.astype(F32))
        at = q_cols + k_cols + j * head_dim
        y = (sums[:, at : at + head_dim] * own_scale).astype(BF16)
        fv_out[:, j * head_dim : (j + 1) * head_dim] = y
        fresh_values.append(y.astype(F32))
    for h in range(heads):
        x = sums[:, h * head_dim : (h + 1) * head_dim]
        x = x * lax.rsqrt(jnp.mean(x * x, axis=1, keepdims=True) + EPS) * query_gain[...]
        at = pl.ds(h, own, stride=heads)
        q_rows[at, :] = x.astype(BF16).astype(F32)
        fk_rows[at, :] = fresh_keys[h // group]
        fv_rows[at, :] = fresh_values[h // group]
        logit = jnp.sum(
            jnp.where(stat_lane == tp * heads + h, stats, 0.0), axis=1, keepdims=True
        )
        bias = jnp.sum(
            jnp.where(bias_lane == tp * heads + h, forget_bias[...], 0.0), axis=1, keepdims=True
        )
        z = logit * own_scale + bias
        log_forget = jnp.minimum(z, 0.0) - jnp.log1p(jnp.exp(-jnp.abs(z)))
        lf_rows[at, :] = jnp.broadcast_to(log_forget, (own, head_dim))

    c_gates.wait()
    row8 = lax.broadcasted_iota(jnp.int32, (8, positions), 0)
    pos8 = lax.broadcasted_iota(jnp.int32, (8, positions), 1)
    row_d = lax.broadcasted_iota(jnp.int32, (8, head_dim), 0)

    def attend(i, carry):
        at = pl.ds(pl.multiple_of(i * 8, 8), 8)
        q = q_rows[at, :]
        q16 = q.astype(BF16)
        self_score = jnp.sum(q * fk_rows[at, :], axis=1, keepdims=True) * factor
        limit = jnp.full((8, positions), 0, jnp.int32)
        for a in range(seqs):
            limit = jnp.where(row8 // heads == a, lengths[i * seqs + a], limit)
        g = jnp.concatenate([gates[i * seqs + a] for a in range(seqs)], axis=0)
        latest = jnp.sum(jnp.where(pos8 == limit - 1, g, 0.0), axis=1, keepdims=True)
        now = latest + lf_rows[at, 0:1]
        cache_copy(i, ck_hbm, ck, k_sem).wait()
        s = jnp.zeros((8, positions), F32)
        for a in range(seqs):
            for j in range(kv_here):
                one = mm_nt(q16, ck[i * seqs + a, j])
                s = jnp.where(row8 // group == a * kv_here + j, one, s)
        s = jnp.where(pos8 < limit, s * factor + now - g, -jnp.inf)
        ceiling = jnp.maximum(jnp.max(s, axis=1, keepdims=True), self_score)
        w = jnp.exp(s - ceiling)
        self_weight = jnp.exp(self_score - ceiling)
        denominator = jnp.sum(w, axis=1, keepdims=True) + self_weight
        w16 = w.astype(BF16)
        cache_copy(i, cv_hbm, cv, v_sem).wait()
        o = jnp.zeros((8, head_dim), F32)
        for a in range(seqs):
            for j in range(kv_here):
                one = mm(w16, cv[i * seqs + a, j])
                o = jnp.where(row_d // group == a * kv_here + j, one, o)
        o_rows[at, :] = (o + self_weight * fv_rows[at, :]) / denominator
        return carry

    lax.fori_loop(0, blocks, attend, 0)

    for h in range(heads):
        ag_buf[ep, :, h * head_dim : (h + 1) * head_dim] = o_rows[
            pl.ds(h, own, stride=heads), :
        ].astype(BF16)
    ep_start(2, lambda p: ag_buf.at[ep], ag_buf)
    c_wo.wait()
    ep_wait(2, lambda p: ag_buf.at[ep], ag_buf)
    ar_buf[tp] = mm(ag_buf[...].reshape(tokens, q_cols), wo[...]).astype(BF16)
    tp_start(0, ar_buf)
    tp_wait(0, ar_buf)
    attn_out = ar_buf[0].astype(F32)
    for p in range(1, t):
        attn_out = attn_out + ar_buf[p].astype(F32)
    middle = (hidden[...].astype(F32) + attn_out).astype(BF16)
    mixed_out[...] = middle
    middle = middle.astype(F32)
    normed_mid = (middle * ffn_gain[:, my_cols]).astype(BF16)

    sq = jnp.sum(middle * middle, axis=1, keepdims=True)
    mix_rows[...] = mix_vector[...].astype(F32)
    share_dot = jnp.zeros((tokens, 1), F32)
    for c in range(width // 128):
        mix_row = mix_rows[pl.ds(ep * (width // 128) + c, 1), :]
        share_dot += jnp.sum(
            normed_mid[:, c * 128 : (c + 1) * 128].astype(F32) * mix_row, axis=1, keepdims=True
        )
    both = jnp.where(lane < 4, sq, share_dot)
    ms_buf[ep] = jnp.transpose(both, (1, 0))[0:8, :]
    ep_start(3, lambda p: ms_buf.at[ep], ms_buf)
    dsp_send[...] = (
        mm(placed_scr[...], normed_mid).astype(BF16).reshape(n, slots_here, width)
    )
    dsp_recv[ep] = dsp_send[ep]
    ep_start(4, lambda p: dsp_send.at[p], dsp_recv)
    c_dg.wait()
    dn_send[:, 0:hidden_units] = mm(normed_mid, dg[...]).astype(BF16)
    c_du.wait()
    dn_send[:, hidden_units:] = mm(normed_mid, du[...]).astype(BF16)
    ep_start(5, own_rows(dn_send), dn_recv)

    ep_wait(3, lambda p: ms_buf.at[ep], ms_buf)
    total = ms_buf[0]
    for p in range(1, n):
        total = total + ms_buf[p]
    mid_row = lax.rsqrt(total[0:1, :] / model + EPS)
    share_row = jax.nn.sigmoid(mid_row * total[4:5, :])
    sub = lax.broadcasted_iota(jnp.int32, (128, tokens), 0)
    col_stats[...] = jnp.transpose(jnp.where(sub < 64, mid_row, share_row), (1, 0))
    slot_at = lax.broadcasted_iota(jnp.int32, (slots_here, tokens), 0) + ep * slots_here
    slot_at = slot_at.astype(F32)
    slot_scale = jnp.zeros((slots_here, 1), F32)
    slot_weight = jnp.zeros((slots_here, 1), F32)
    for k in range(TOPK):
        hit = slot_at == slot_rows[k : k + 1, :]
        slot_scale += jnp.sum(jnp.where(hit, mid_row, 0.0), axis=1, keepdims=True)
        slot_weight += jnp.sum(
            jnp.where(hit, route_weight[k : k + 1, :], 0.0), axis=1, keepdims=True
        )

    c_eg.wait()
    c_eu.wait()
    c_ed.wait()
    ep_wait(4, lambda p: dsp_send.at[p], dsp_recv)
    arrived = jnp.concatenate([dsp_recv[p] for p in range(n)], axis=1)

    def by_expert(results):
        row = lax.broadcasted_iota(jnp.int32, results[0].shape, 0)
        out = results[0]
        for e in range(1, local_experts):
            out = jnp.where(row >= e * CAPACITY, results[e], out)
        return out

    gate_pre = by_expert([mm(arrived, eg[e]) for e in range(local_experts)]) * slot_scale
    up_pre = by_expert([mm(arrived, eu[e]) for e in range(local_experts)]) * slot_scale
    expert_hidden = (jax.nn.silu(gate_pre) * up_pre).astype(BF16)
    for p in range(n):
        cols = slice(p * width, (p + 1) * width)
        part = by_expert([mm(expert_hidden, ed[e, :, cols]) for e in range(local_experts)])
        ret_send[p] = (part * slot_weight).astype(BF16)
    ret_recv[ep] = ret_send[ep]
    ep_start(6, lambda p: ret_send.at[p], ret_recv)

    ep_wait(5, own_rows(dn_send), dn_recv)
    my_rows = pl.ds(pl.multiple_of(ep * own, own), own)
    dense = dn_send[my_rows, :].astype(F32)
    for p in ep_peers:
        dense = dense + dn_recv[p].astype(F32)
    own_mid = col_stats[my_rows, 0:1]
    dh_buf[ep] = (
        jax.nn.silu(dense[:, 0:hidden_units] * own_mid) * (dense[:, hidden_units:] * own_mid)
    ).astype(BF16)
    ep_start(7, lambda p: dh_buf.at[ep], dh_buf)
    c_dd.wait()
    ep_wait(6, lambda p: ret_send.at[p], ret_recv)
    routed = mm(placed_t[...], ret_recv[...].reshape(slots, width))
    ep_wait(7, lambda p: dh_buf.at[ep], dh_buf)
    dense_part = mm(dh_buf[...].reshape(tokens, hidden_units), dd[...])
    ar2_buf[tp] = (routed + col_stats[:, 127:128] * dense_part).astype(BF16)
    tp_start(1, ar2_buf)
    tp_wait(1, ar2_buf)
    ffn = ar2_buf[0].astype(F32)
    for p in range(1, t):
        ffn = ffn + ar2_buf[p].astype(F32)
    mixed_out[...] = (mixed_out[...].astype(F32) + ffn).astype(BF16)


def hand_over(mixed, fresh_keys, fresh_values, mixed_out, fk_out, fv_out):
    mixed_out[...] = mixed[...]
    fk_out[...] = fresh_keys[...]
    fv_out[...] = fresh_values[...]


def on_device(
    hidden_in,
    attn_gain,
    forget_weight,
    forget_bias,
    query_weight,
    key_weight,
    value_weight,
    query_gain,
    key_gain,
    cache_keys,
    cache_values,
    cache_gates,
    lengths,
    output_weight,
    ffn_gain,
    route_group,
    route_expert,
    route_weight,
    expert_gate,
    expert_up,
    expert_down,
    mix_vector,
    dense_gate,
    dense_up,
    dense_down,
):
    n = lax.axis_size("ep")
    t = lax.axis_size("tp")
    tokens, width = hidden_in.shape
    own, kv_here, positions, head_dim = cache_keys.shape
    q_cols = query_weight.shape[1]
    k_cols = key_weight.shape[1]
    heads = q_cols // head_dim
    units = dense_gate.shape[1]
    slots_here = expert_gate.shape[0] * CAPACITY
    slots = n * slots_here
    rows = own * heads
    blocks = rows // 8

    def vm(shape, dtype):
        return pltpu.VMEM(shape, dtype)

    def like(x):
        return pltpu.VMEM(x.shape, x.dtype)

    big = [
        forget_weight.T,
        query_weight,
        key_weight,
        value_weight,
        cache_keys,
        cache_values,
        cache_gates,
        output_weight,
        expert_gate,
        expert_up,
        expert_down,
        dense_gate,
        dense_up,
        dense_down,
    ]
    small = [
        hidden_in,
        attn_gain[None],
        forget_bias[None],
        query_gain[None],
        key_gain[None],
        ffn_gain[None],
        mix_vector.reshape(-1, 128),
        route_group[None],
        route_expert.T,
        route_weight.T,
    ]
    vmem = pl.BlockSpec(memory_space=pltpu.VMEM)
    out_shape = (
        jax.ShapeDtypeStruct((tokens, width), BF16),
        jax.ShapeDtypeStruct((own, k_cols), BF16),
        jax.ShapeDtypeStruct((own, k_cols), BF16),
    )
    results = pl.pallas_call(
        functools.partial(layer_kernel, n, t),
        out_shape=out_shape,
        in_specs=[vmem] * len(small)
        + [pl.BlockSpec(memory_space=pltpu.SMEM)]
        + [pl.BlockSpec(memory_space=pl.ANY)] * len(big),
        out_specs=(vmem, vmem, vmem),
        scratch_shapes=[vm((forget_weight.shape[1], width), BF16)]
        + [like(x) for x in big[1:]]
        + [vm((rows, head_dim), F32)] * 5
        + [
            vm((n * width // 128, 128), F32),
            vm((slots, tokens), BF16),
            vm((tokens, slots), BF16),
            vm((8, tokens), F32),
            vm((tokens, q_cols + 2 * k_cols), BF16),
            vm((n, own, q_cols + 2 * k_cols), BF16),
            vm((tokens, 128), F32),
            vm((n, own, 128), F32),
            vm((n, own, q_cols), BF16),
            vm((t, tokens, width), BF16),
            vm((n, 8, tokens), F32),
            vm((tokens, 128), F32),
            vm((n, slots_here, width), BF16),
            vm((n, slots_here, width), BF16),
            vm((tokens, 2 * units), BF16),
            vm((n, own, 2 * units), BF16),
            vm((n, slots_here, width), BF16),
            vm((n, slots_here, width), BF16),
            vm((n, own, units), BF16),
            vm((t, tokens, width), BF16),
            pltpu.SemaphoreType.DMA((12,)),
            pltpu.SemaphoreType.DMA((blocks,)),
            pltpu.SemaphoreType.DMA((blocks,)),
            pltpu.SemaphoreType.DMA((8, n)),
            pltpu.SemaphoreType.DMA((8, n)),
            pltpu.SemaphoreType.DMA((2, t)),
            pltpu.SemaphoreType.DMA((2, t)),
        ],
        compiler_params=pltpu.CompilerParams(
            collective_id=0, has_side_effects=True, vmem_limit_bytes=58 * 1024 * 1024
        ),
    )(*small, lengths, *big)
    return pl.pallas_call(
        hand_over, out_shape=out_shape, in_specs=[vmem] * 3, out_specs=(vmem, vmem, vmem)
    )(*results)


def solution(mesh):
    placed = (
        P(None, "ep"),
        P(),
        P(),
        P(),
        P("ep", "tp"),
        P("ep", "tp"),
        P("ep", "tp"),
        P(),
        P(),
        P("ep", "tp", None, None),
        P("ep", "tp", None, None),
        P("ep", "tp", None),
        P("ep"),
        P("tp", "ep"),
        P(),
        P(),
        P(),
        P(),
        P("ep", None, "tp"),
        P("ep", None, "tp"),
        P("ep", "tp", None),
        P(),
        P("ep", "tp"),
        P("ep", "tp"),
        P("tp", "ep"),
    )
    return jax.shard_map(
        on_device,
        mesh=mesh,
        in_specs=placed,
        out_specs=(P(None, "ep"), P("ep", "tp"), P("ep", "tp")),
        check_vma=False,
    )
```
